256 devices in a mesh: sp: 32 (over z, x), tp: 8 (over y, core).
Axes of the slice: x: 4, y: 4, z: 8, core: 2. Of those that a mesh axis runs over, the one named last changes fastest.
Arguments:
- stream: bfloat16 [32768, 2048], P(('sp', 'tp')), may hold values from -6 to 6
- mixer_input: bfloat16 [32768, 1024], P('sp', 'tp'), may hold values from -6 to 6
- document_ids: int32 [32768], P('sp'), may hold values from 0 to 15, never falling along the last dimension, each value on 1 to 4096 neighbouring positions
- decay_rate: float32 [64, 64], P('tp'), may hold values from 6.1035156e-05 to 0.015625
- rotation: float32 [64, 64], P('tp'), may hold values from -3.140625 to 3.140625
- forget_log: float32 [32768, 64], P('sp', 'tp'), may hold values from -1 to 0
- input_map: bfloat16 [2, 64, 64, 16], P(None, 'tp'), may hold values from -1.5 to 1.5
- readout_map: bfloat16 [2, 64, 16, 64], P(None, 'tp'), may hold values from -0.5 to 0.5
- skip_gain: float32 [64, 16], P('tp'), may hold values from -3 to 3
- out_projection: bfloat16 [1024, 2048], replicated, may hold values from -0.1875 to 0.1875
- norm_gain: float32 [2048], replicated, may hold values from 0.1 to 1.9
- expert_ids: int32 [32768, 8], P('sp'), may hold values from 0 to 255, all different within a row; in each aligned block of 1024 rows (0 to 1023, 1024 to 2047, ...) at most 64 rows name the same one
- route_weight: float32 [32768, 8], P('sp'), may hold values from 0.05 to 1
- expert_gate: bfloat16 [256, 2048, 512], P(('sp', 'tp')), may hold values from -0.125 to 0.125
- expert_up: bfloat16 [256, 2048, 512], P(('sp', 'tp')), may hold values from -0.125 to 0.125
- expert_down: bfloat16 [256, 512, 2048], P(('sp', 'tp')), may hold values from -0.25 to 0.25
- shared_gate: bfloat16 [2048, 512], P(None, 'tp'), may hold values from -0.125 to 0.125
- shared_up: bfloat16 [2048, 512], P(None, 'tp'), may hold values from -0.125 to 0.125
- shared_down: bfloat16 [512, 2048], P('tp'), may hold values from -0.25 to 0.25
Outputs:
- layer_out: bfloat16 [32768, 2048], P(('sp', 'tp'))
The draws below stay inside these ranges and needn't reach their ends.
Inputs may be any that keep to these rules, and one draw needn't show every extreme that they name: `expert_ids`: each row names 8 different experts. In the rows of one device (aligned blocks of 1024 rows) no expert is named by more than 64 rows. `document_ids`: never falling along the positions; each document covers 1 to 4096 positions.
All inputs are finite; a program needn't handle non-finite values.
Results may differ from the reference program's by a relative error of at most 0.018.
Values may be sent and summed in bfloat16 or wider, within the bound.
A program may use at most 256 MiB of HBM per device.

```python
import math
import jax
import jax.numpy as jnp
import numpy as np
from jax import lax

D = 2048
SSM_WIDTH = 1024
GROUP = 16
STATE = 64
EFF = 512
SFF = 512
TOP_K = 8
TOK_DEV = 1024
TOKEN_POSITIONS = 32768
SSM_GROUPS = 64
EXPERTS = 256
CAP = 64
DOCS = 16
DOC_MOST = 4096
N_SP = 32
N_TP = 8


def draw_decay_rate(key, part):
    random_key_split = jax.random.split(key, 3)
    fast_share = 0.5
    is_fast = jax.random.uniform(random_key_split[0], (SSM_GROUPS, STATE), jnp.float32) < fast_share
    fast_rate = jnp.exp(jax.random.uniform(random_key_split[1], (SSM_GROUPS, STATE), jnp.float32, math.log(4.0 / TOK_DEV), math.log(16.0 / TOK_DEV)))
    slow_rate = jnp.exp(jax.random.uniform(random_key_split[2], (SSM_GROUPS, STATE), jnp.float32, math.log(0.25 / DOC_MOST), math.log(1.0 / DOC_MOST)))
    return jnp.where(is_fast, fast_rate, slow_rate).astype(jnp.float32)


def draw_forget_log(key, part):
    random_key_split = jax.random.split(key, 4)
    blocks = TOKEN_POSITIONS // TOK_DEV
    lowest_factor = 0.2
    highest_factor = 3.0
    factor = jnp.exp(jax.random.uniform(random_key_split[0], (blocks, SSM_GROUPS), jnp.float32, math.log(lowest_factor), math.log(highest_factor)))
    factor = jnp.repeat(factor, TOK_DEV, axis=0)
    roughness = jax.random.uniform(random_key_split[1], (TOKEN_POSITIONS, SSM_GROUPS), jnp.float32, 0.5, 1.5)
    reference_level = -factor * roughness / DOC_MOST
    spike_location = jax.random.randint(random_key_split[2], (3,), 0, TOKEN_POSITIONS)
    spike_flag = jnp.any(jnp.arange(TOKEN_POSITIONS)[:, None] == spike_location[None, :], axis=1)
    spike_amplitude = jax.random.uniform(random_key_split[3], (TOKEN_POSITIONS, 1), jnp.float32, math.log(0.5), math.log(0.8))
    return jnp.where(spike_flag[:, None], reference_level + spike_amplitude, reference_level).astype(jnp.float32)


def block_levels(own_key, dims, cuts, low, largest):
    def one(dim, shards_of):
        draws = jax.random.uniform(jax.random.fold_in(jax.random.fold_in(own_key, 6), dim), (shards_of,), jnp.float32, low / len(cuts), largest / len(cuts))
        return jnp.repeat(jnp.exp(draws), dims[dim] // shards_of).reshape((-1,) + (1,) * (len(dims) - dim - 1))

    level = one(*cuts[0])
    for cut in cuts[1:]:
        level = level * one(*cut)
    return level


def length_profile(count, total, bound, slope):
    loads = [(1 << 20) // math.isqrt(standing ** slope) + 1 for standing in range(2, count + 1)]
    spare, given = total - bound - (count - 1), [1] * (count - 1)
    while spare > 0:
        free = [i for i in range(count - 1) if given[i] < bound]
        pool, budget = sum([loads[i] for i in free]), spare
        for i in free:
            more = min(bound - given[i], max(1, budget * loads[i] // pool), spare)
            given[i] = given[i] + more
            spare = spare - more
    return np.array([bound] + given)


def ragged(stream_key, amount, total, most, lean):
    if amount == 2:
        one = jax.random.randint(stream_key, (), max(1, total - most), min(most, total - 1) + 1)
        return jnp.stack([one, total - one])
    sizes = jnp.asarray(length_profile(amount, total, most, lean), jnp.int32)
    couples = (amount - 1) // 2
    giver, taker = sizes[1:1 + 2 * couples:2], sizes[2:2 + 2 * couples:2]
    slack = jnp.minimum(giver - 1, most - taker)
    shifted = jax.random.randint(jax.random.fold_in(stream_key, 1), (couples,), 0, 1 << 20) % (slack + 1)
    sizes = sizes.at[1:1 + 2 * couples:2].set(giver - shifted).at[2:2 + 2 * couples:2].set(taker + shifted)
    return sizes[jax.random.permutation(jax.random.fold_in(stream_key, 2), amount)]


def deal_out(stream_key, own, number, rows, count, top, reach, skew):
    sequence = jax.random.permutation(stream_key, count)
    crowded, common = portions_of(count, rows * top, reach, skew, True), portions_of(count, rows * top, reach, skew, False)
    places = jnp.arange(count)

    def named(tallies, turn):
        used = int((tallies > 0).sum())
        fixed = max(1, used // 4)
        moved = fixed + (places - fixed + turn * (used - fixed)) % max(1, count - fixed)
        return jnp.zeros((count,), jnp.int32).at[sequence[jnp.where(places < fixed, places, moved)]].set(jnp.asarray(tallies, jnp.int32))

    tallies = jnp.where(number % 4 == 0, named(crowded, number // 4), named(common, number - number // 4 - 1))
    mixed = jax.random.permutation(jax.random.fold_in(own, 3), count)
    giver, receiver = mixed[0:count // 2 * 2:2], mixed[1:count // 2 * 2:2]
    margin = jnp.minimum(tallies[giver] - 1, reach - tallies[receiver]) // 2
    margin = jnp.where((giver == sequence[0]) | (receiver == sequence[0]) | (tallies[receiver] == 0), 0, jnp.maximum(margin, 0))
    moved = jax.random.randint(jax.random.fold_in(own, 4), (count // 2,), 0, 1 << 20) % (margin + 1)
    tallies = tallies.at[giver].add(-moved).at[receiver].add(moved)
    items = jnp.searchsorted(jnp.cumsum(tallies), jnp.arange(rows * top), side="right").astype(jnp.int32)
    grid = items.reshape(top, rows).T
    grid = grid[jax.random.permutation(jax.random.fold_in(own, 1), rows)]
    turn = jax.random.randint(jax.random.fold_in(own, 2), (rows, 1), 0, top)
    return jnp.take_along_axis(grid, (jnp.arange(top)[None, :] + turn) % top, axis=1)


def portions_of(count, total, most, skew, full):
    portions = [(1 << 20) // math.isqrt(rank ** skew) + 1 for rank in range(1, count + 1)]
    largest = most if full else min(most, max(-(-total // count), total * portions[0] // sum(portions)))
    least = 1 if total - largest >= count - 1 else 0
    given, surplus = [largest] + [least] * (count - 1), total - largest - least * (count - 1)
    while surplus > 0:
        free = [i for i in range(1, count) if given[i] < largest] or [i for i in range(1, count) if given[i] < most]
        whole, remaining = sum([portions[i] for i in free]), surplus
        for i in free:
            more = min(most - given[i], max(1, remaining * portions[i] // whole), surplus)
            given[i] = given[i] + more
            surplus = surplus - more
    return np.array(given)


def bell_draw(own_key, extent, spread, bound, cuts=(), kind=jnp.bfloat16):
    values = spread * jax.random.normal(own_key, extent, jnp.float32)
    if cuts:
        values = values * block_levels(own_key, extent, cuts, -0.22, 0.18)
    return jnp.clip(values, -bound, bound).astype(kind)


def setup_inputs(seed: int = 0) -> dict:
    arg_keys = jax.random.split(jax.random.key(seed), 20)
    stream = bell_draw(arg_keys[0], (TOKEN_POSITIONS, D), 1.0, 6.0, ((0, 256),))
    mixer_input = bell_draw(arg_keys[1], (TOKEN_POSITIONS, SSM_WIDTH), 1.0, 6.0, ((0, 32), (1, 8)))
    document_ids = jnp.searchsorted(jnp.cumsum(ragged(arg_keys[2], DOCS, TOKEN_POSITIONS, DOC_MOST, 2)), jnp.arange(TOKEN_POSITIONS), side="right").astype(jnp.int32)
    decay_rate = draw_decay_rate(jax.random.fold_in(arg_keys[19], 71), 0)
    rotation = jnp.clip(jax.random.uniform(arg_keys[4], (SSM_GROUPS, STATE), jnp.float32, -3.140625, 3.140625), -3.140625, 3.140625)
    forget_log = draw_forget_log(jax.random.fold_in(arg_keys[19], 71), 0)
    input_map = bell_draw(arg_keys[6], (2, SSM_GROUPS, STATE, GROUP), GROUP ** -0.5, 1.5, ((1, 8),))
    readout_map = bell_draw(arg_keys[7], (2, SSM_GROUPS, GROUP, STATE), (2 * STATE) ** -0.5, 0.5, ((1, 8),))
    skip_gain = bell_draw(arg_keys[8], (SSM_GROUPS, GROUP), 0.5, 3.0, ((0, 8),), jnp.float32)
    out_projection = bell_draw(arg_keys[9], (SSM_WIDTH, D), SSM_WIDTH ** -0.5, 0.1875)
    norm_gain = jnp.clip(1.0 + 0.18 * jax.random.normal(arg_keys[10], (D,), jnp.float32), 0.1, 1.9)
    expert_ids_keys = jax.random.split(jax.random.fold_in(arg_keys[11], 1), TOKEN_POSITIONS // TOK_DEV)
    expert_ids_turns = jax.random.permutation(jax.random.fold_in(arg_keys[11], 3), TOKEN_POSITIONS // TOK_DEV)
    expert_ids = jax.vmap(lambda own, number: deal_out(jax.random.fold_in(arg_keys[11], 2), own, number, TOK_DEV, EXPERTS, TOP_K, CAP, 2))(expert_ids_keys, expert_ids_turns).reshape((TOKEN_POSITIONS, TOP_K))
    route_weight = jnp.clip(jnp.exp(math.log(1.0) - 2.9957323 * jax.random.uniform(arg_keys[12], (TOKEN_POSITIONS, TOP_K), jnp.float32) ** block_levels(arg_keys[12], (TOKEN_POSITIONS, TOP_K), ((0, 32),), -0.2, 0.2)), 0.05, 1.0)
    expert_gate = bell_draw(arg_keys[13], (EXPERTS, D, EFF), D ** -0.5, 0.125, ((0, 256),))
    expert_up = bell_draw(arg_keys[14], (EXPERTS, D, EFF), D ** -0.5, 0.125, ((0, 256),))
    expert_down = bell_draw(arg_keys[15], (EXPERTS, EFF, D), EFF ** -0.5, 0.25, ((0, 256),))
    shared_gate = bell_draw(arg_keys[16], (D, SFF), D ** -0.5, 0.125, ((1, 8),))
    shared_up = bell_draw(arg_keys[17], (D, SFF), D ** -0.5, 0.125, ((1, 8),))
    shared_down = bell_draw(arg_keys[18], (SFF, D), SFF ** -0.5, 0.25, ((0, 8),))
    return dict(stream=stream, mixer_input=mixer_input, document_ids=document_ids, decay_rate=decay_rate, rotation=rotation, forget_log=forget_log, input_map=input_map, readout_map=readout_map, skip_gain=skip_gain, out_projection=out_projection, norm_gain=norm_gain, expert_ids=expert_ids, route_weight=route_weight, expert_gate=expert_gate, expert_up=expert_up, expert_down=expert_down, shared_gate=shared_gate, shared_up=shared_up, shared_down=shared_down)


norm_eps = 1e-06
highest = lax.Precision.HIGHEST

def pair_combine(earlier, later):
    a_re1, a_im1, b_re1, b_im1 = earlier
    a_re2, a_im2, b_re2, b_im2 = later
    return (a_re1 * a_re2 - a_im1 * a_im2, a_re1 * a_im2 + a_im1 * a_re2, a_re2 * b_re1 - a_im2 * b_im1 + b_re2, a_re2 * b_im1 + a_im2 * b_re1 + b_im2)

def reference(stream, mixer_input, document_ids, decay_rate, rotation, forget_log, input_map, readout_map, skip_gain, out_projection, norm_gain, expert_ids, route_weight, expert_gate, expert_up, expert_down, shared_gate, shared_up, shared_down):
    starts = jnp.concatenate([jnp.zeros((1,), bool), document_ids[1:] != document_ids[:-1]])
    input_f = mixer_input.astype(jnp.float32)
    grouped = input_f.reshape(TOKEN_POSITIONS, SSM_GROUPS, GROUP).transpose(1, 0, 2)
    in_maps = input_map.astype(jnp.float32).transpose(1, 0, 2, 3)
    out_maps = readout_map.astype(jnp.float32).transpose(1, 0, 2, 3)

    def group_scan(pieces):
        input_g, forget_g, rate_g, turn_g, in_g, out_g, skip_g = pieces
        magnitude = jnp.exp(forget_g[:, None] - rate_g[None, :])
        decay_re = jnp.where(starts[:, None], 0.0, magnitude * jnp.cos(turn_g)[None, :])
        decay_im = jnp.where(starts[:, None], 0.0, magnitude * jnp.sin(turn_g)[None, :])
        in_scale = jnp.sqrt(1.0 - jnp.exp(-2.0 * rate_g))
        driven_re = jnp.dot(input_g, in_g[0].T, precision=highest) * in_scale[None, :]
        driven_im = jnp.dot(input_g, in_g[1].T, precision=highest) * in_scale[None, :]
        scanned = lax.associative_scan(pair_combine, (decay_re, decay_im, driven_re, driven_im), axis=0)
        readout = jnp.dot(scanned[2], out_g[0].T, precision=highest) - jnp.dot(scanned[3], out_g[1].T, precision=highest) + skip_g[None, :] * input_g
        return jax.nn.gelu(readout)
    mixer_rows = lax.map(group_scan, (grouped, forget_log.T, decay_rate, rotation, in_maps, out_maps, skip_gain))
    mixer_out = mixer_rows.transpose(1, 0, 2).reshape(TOKEN_POSITIONS, SSM_WIDTH).astype(jnp.bfloat16)
    mixed = jnp.dot(mixer_out.astype(jnp.float32), out_projection.astype(jnp.float32))
    residual = (stream.astype(jnp.float32) + mixed).astype(jnp.bfloat16)
    resid_f = residual.astype(jnp.float32)
    normed = (resid_f * lax.rsqrt(lax.optimization_barrier(jnp.mean(resid_f * resid_f, axis=-1, keepdims=True)) + norm_eps) * norm_gain[None, :]).astype(jnp.bfloat16)
    normed_f = normed.astype(jnp.float32)
    normed_pad = jnp.concatenate([normed_f, jnp.zeros((1, D), jnp.float32)])
    flat_expert = expert_ids.reshape(-1).astype(jnp.int32)
    flat_weight = route_weight.reshape(-1)
    sorted_slots = jnp.argsort(flat_expert, stable=True).astype(jnp.int32)
    counts = jnp.bincount(flat_expert, length=EXPERTS).astype(jnp.int32)
    offsets = (jnp.cumsum(counts) - counts).astype(jnp.int32)
    slot_range = jnp.arange(N_SP * CAP, dtype=jnp.int32)

    def expert_pass(expert, routed_sum):
        is_live = slot_range < counts[expert]
        position = sorted_slots[jnp.minimum(offsets[expert] + slot_range, TOKEN_POSITIONS * TOP_K - 1)]
        token_table = jnp.where(is_live, position // TOP_K, TOKEN_POSITIONS).astype(jnp.int32)
        weight_table = jnp.where(is_live, flat_weight[position], 0.0)
        row_block = normed_pad[token_table]
        gate_value = jnp.dot(row_block, expert_gate[expert].astype(jnp.float32))
        up_value = jnp.dot(row_block, expert_up[expert].astype(jnp.float32))
        hidden = lax.optimization_barrier((jax.nn.silu(gate_value) * up_value).astype(jnp.bfloat16))
        expert_rows = jnp.dot(hidden.astype(jnp.float32), expert_down[expert].astype(jnp.float32)).astype(jnp.bfloat16)
        return routed_sum.at[token_table].add(weight_table[:, None] * expert_rows.astype(jnp.float32), mode='drop')
    block_width = SFF // N_TP
    total = resid_f
    for column in range(N_TP):
        routed_sum = lax.fori_loop(0, N_SP, lambda source, acc_sum: expert_pass(source * N_TP + column, acc_sum), jnp.zeros((TOKEN_POSITIONS, D), jnp.float32))
        lower = column * block_width
        gate_block = jnp.dot(normed_f, shared_gate[:, lower:lower + block_width].astype(jnp.float32))
        up_block = jnp.dot(normed_f, shared_up[:, lower:lower + block_width].astype(jnp.float32))
        shared_hidden = lax.optimization_barrier((jax.nn.silu(gate_block) * up_block).astype(jnp.bfloat16))
        shared_part = jnp.dot(shared_hidden.astype(jnp.float32), shared_down[lower:lower + block_width].astype(jnp.float32))
        partial_value = lax.optimization_barrier((routed_sum + shared_part).astype(jnp.bfloat16))
        total = total + partial_value.astype(jnp.float32)
    return total.astype(jnp.bfloat16)
```

```python
import functools
import jax
import jax.numpy as jnp
from jax import lax
from jax.experimental import pallas as pl
from jax.experimental.pallas import tpu as pltpu
from jax.sharding import Mesh, PartitionSpec as P

norm_eps = 1e-06
highest = lax.Precision.HIGHEST
lanes_of_blocks = 8
reach = 4


def expand_gain(gain_ref, states):
    groups = gain_ref.shape[1]
    wide = groups * states
    lane_group = lax.broadcasted_iota(jnp.int32, (groups, wide), 1) // states
    row_group = lax.broadcasted_iota(jnp.int32, (groups, wide), 0)
    spread = jnp.where(lane_group == row_group, 1.0, 0.0).astype(jnp.float32)
    return jnp.dot(gain_ref[...], spread, precision=highest, preferred_element_type=jnp.float32)


def drive(input_ref, map_ref, scale_ref, gain_ref, driven, gain, states):
    rows = input_ref.shape[0]
    order_row = lax.broadcasted_iota(jnp.int32, (rows, rows), 0)
    order_col = lax.broadcasted_iota(jnp.int32, (rows, rows), 1)
    steps = rows // lanes_of_blocks
    source = (order_row % lanes_of_blocks) * steps + order_row // lanes_of_blocks
    pick = jnp.where(source == order_col, 1.0, 0.0).astype(jnp.bfloat16)
    stepped = jnp.dot(pick, input_ref[...], preferred_element_type=jnp.float32).astype(jnp.bfloat16)
    driven[...] = (
        jnp.dot(stepped, map_ref[...], preferred_element_type=jnp.float32) * scale_ref[...]
    )
    gain[...] = expand_gain(gain_ref, states)


def block_summary(states, input_ref, map_ref, scale_ref, gain_ref, turn_ref, out_ref, driven, gain):
    drive(input_ref, map_ref, scale_ref, gain_ref, driven, gain, states)
    wide = turn_ref.shape[1]
    steps = input_ref.shape[0] // lanes_of_blocks
    shape = (lanes_of_blocks, wide)
    turn_re = jnp.broadcast_to(turn_ref[0:1], shape)
    turn_im = jnp.broadcast_to(turn_ref[1:2], shape)

    def one(step, held):
        p_re, p_im, s_re, s_im = held
        rows = pl.ds(pl.multiple_of(step * lanes_of_blocks, lanes_of_blocks), lanes_of_blocks)
        g = gain[rows, :]
        a_re = g * turn_re
        a_im = g * turn_im
        return (
            a_re * p_re - a_im * p_im,
            a_re * p_im + a_im * p_re,
            a_re * s_re - a_im * s_im + driven[rows, :wide],
            a_re * s_im + a_im * s_re + driven[rows, wide:],
        )

    ones = jnp.ones(shape, jnp.float32)
    zero = jnp.zeros(shape, jnp.float32)
    last = lax.fori_loop(0, steps, one, (ones, zero, zero, zero), unroll=4)
    for k in range(4):
        out_ref[k] = last[k]


def read_out(
    states, input_ref, map_ref, scale_ref, gain_ref, turn_ref, enter_ref, readout_ref, skip_ref,
    out_ref, driven, gain,
):
    drive(input_ref, map_ref, scale_ref, gain_ref, driven, gain, states)
    wide = turn_ref.shape[1]
    rows_all = input_ref.shape[0]
    steps = rows_all // lanes_of_blocks
    shape = (lanes_of_blocks, wide)
    turn_re = jnp.broadcast_to(turn_ref[0:1], shape)
    turn_im = jnp.broadcast_to(turn_ref[1:2], shape)

    def one(step, held):
        s_re, s_im = held
        rows = pl.ds(pl.multiple_of(step * lanes_of_blocks, lanes_of_blocks), lanes_of_blocks)
        g = gain[rows, :]
        a_re = g * turn_re
        a_im = g * turn_im
        n_re = a_re * s_re - a_im * s_im + driven[rows, :wide]
        n_im = a_re * s_im + a_im * s_re + driven[rows, wide:]
        driven[rows, :wide] = n_re
        driven[rows, wide:] = n_im
        return n_re, n_im

    lax.fori_loop(0, steps, one, (enter_ref[0], enter_ref[1]), unroll=4)
    full = driven[...]
    high = full.astype(jnp.bfloat16)
    low = (full - high.astype(jnp.float32)).astype(jnp.bfloat16)
    stepped = jnp.dot(high, readout_ref[...], preferred_element_type=jnp.float32) + jnp.dot(
        low, readout_ref[...], preferred_element_type=jnp.float32
    )
    s_high = stepped.astype(jnp.bfloat16)
    s_low = (stepped - s_high.astype(jnp.float32)).astype(jnp.bfloat16)
    order_row = lax.broadcasted_iota(jnp.int32, (rows_all, rows_all), 0)
    order_col = lax.broadcasted_iota(jnp.int32, (rows_all, rows_all), 1)
    source = (order_row % steps) * lanes_of_blocks + order_row // steps
    pick = jnp.where(source == order_col, 1.0, 0.0).astype(jnp.bfloat16)
    natural = jnp.dot(pick, s_high, preferred_element_type=jnp.float32) + jnp.dot(
        pick, s_low, preferred_element_type=jnp.float32
    )
    natural = natural + skip_ref[...] * input_ref[...].astype(jnp.float32)
    out_ref[...] = jax.nn.gelu(natural).astype(jnp.bfloat16)


vmem = pl.BlockSpec(memory_space=pltpu.VMEM)


def mixer(mixer_input, document_ids, decay_rate, rotation, forget_log, input_map, readout_map, skip_gain):
    rows, channels = mixer_input.shape
    groups, states = decay_rate.shape
    size = channels // groups
    wide = groups * states
    steps = rows // lanes_of_blocks
    own = jnp.eye(groups, dtype=jnp.bfloat16)
    map_wide = jnp.einsum("cgph,gk->ghckp", input_map, own).reshape(channels, 2 * wide)
    readout_wide = jnp.einsum(
        "cghp,gk->cgpkh", readout_map * jnp.array([1, -1], jnp.bfloat16)[:, None, None, None], own
    ).reshape(2 * wide, channels)
    scale = jnp.sqrt(1.0 - jnp.exp(-2.0 * decay_rate)).reshape(1, wide)
    scale = jnp.concatenate([scale, scale], axis=1)
    magnitude = jnp.exp(-decay_rate)
    turn = jnp.stack(
        [(magnitude * jnp.cos(rotation)).reshape(-1), (magnitude * jnp.sin(rotation)).reshape(-1)]
    )
    starts = jnp.concatenate([jnp.zeros((1,), bool), document_ids[1:] != document_ids[:-1]])
    gain = jnp.where(starts[:, None], 0.0, jnp.exp(forget_log))
    gain = gain.reshape(lanes_of_blocks, steps, groups).transpose(1, 0, 2).reshape(rows, groups)
    skip = skip_gain.reshape(1, channels)
    scratch = [pltpu.VMEM((rows, 2 * wide), jnp.float32), pltpu.VMEM((rows, wide), jnp.float32)]
    params = pltpu.CompilerParams(vmem_limit_bytes=48 * 1024 * 1024)
    ends = pl.pallas_call(
        functools.partial(block_summary, states),
        out_shape=jax.ShapeDtypeStruct((4, lanes_of_blocks, wide), jnp.float32),
        in_specs=[vmem] * 5,
        out_specs=vmem,
        scratch_shapes=scratch,
        compiler_params=params,
        name="block_summary",
    )(mixer_input, map_wide, scale, gain, turn)

    p_re, p_im, s_re, s_im = ends
    a_re, a_im = jnp.ones((wide,), jnp.float32), jnp.zeros((wide,), jnp.float32)
    b_re, b_im = jnp.zeros((wide,), jnp.float32), jnp.zeros((wide,), jnp.float32)
    for k in range(lanes_of_blocks):
        a_re, a_im = p_re[k] * a_re - p_im[k] * a_im, p_re[k] * a_im + p_im[k] * a_re
        b_re, b_im = (
            p_re[k] * b_re - p_im[k] * b_im + s_re[k],
            p_re[k] * b_im + p_im[k] * b_re + s_im[k],
        )
    first_doc = document_ids[0].astype(jnp.float32)
    last_doc = document_ids[-1].astype(jnp.float32)
    first_row = jnp.full((wide,), 1.0, jnp.float32) * first_doc
    last_row = jnp.full((wide,), 1.0, jnp.float32) * last_doc
    summary = jnp.stack([a_re, a_im, b_re, b_im, first_row, last_row, first_row, last_row])
    shards = lax.axis_size("z") * lax.axis_size("x")
    me = lax.axis_index("z") * lax.axis_size("x") + lax.axis_index("x")
    earlier = [
        lax.ppermute(summary, ("z", "x"), [(i, (i + k) % shards) for i in range(shards)])
        for k in range(1, reach + 1)
    ]
    e_re, e_im = jnp.zeros((wide,), jnp.float32), jnp.zeros((wide,), jnp.float32)
    for k in range(reach, 0, -1):
        before = earlier[k - 1]
        t_re = before[0] * e_re - before[1] * e_im + before[2]
        t_im = before[0] * e_im + before[1] * e_re + before[3]
        after = earlier[k - 2][4] if k > 1 else first_row
        joined = (before[5] == after) & (me >= k)
        e_re = jnp.where(joined, t_re, 0.0)
        e_im = jnp.where(joined, t_im, 0.0)
    enter = []
    for k in range(lanes_of_blocks):
        enter.append((e_re, e_im))
        e_re, e_im = (
            p_re[k] * e_re - p_im[k] * e_im + s_re[k],
            p_re[k] * e_im + p_im[k] * e_re + s_im[k],
        )
    enter = jnp.stack([jnp.stack([e[0] for e in enter]), jnp.stack([e[1] for e in enter])])
    return pl.pallas_call(
        functools.partial(read_out, states),
        out_shape=jax.ShapeDtypeStruct((rows, channels), jnp.bfloat16),
        in_specs=[vmem] * 8,
        out_specs=vmem,
        scratch_shapes=scratch,
        compiler_params=params,
        name="read_out",
    )(mixer_input, map_wide, scale, gain, turn, enter, readout_wide, skip)


def body(
    stream,
    mixer_input,
    document_ids,
    decay_rate,
    rotation,
    forget_log,
    input_map,
    readout_map,
    skip_gain,
    out_projection,
    norm_gain,
    expert_ids,
    route_weight,
    expert_gate,
    expert_up,
    expert_down,
    shared_gate,
    shared_up,
    shared_down,
):
    column = lax.axis_index("tp")
    plane = lax.axis_index("z")
    peers = lax.axis_size("x") * lax.axis_size("tp")
    token_count, route_count = expert_ids.shape
    capacity = max(2, 2 * token_count * route_count // (lax.axis_size("z") * peers))

    gate_all = lax.all_gather(shared_gate, "tp", axis=1, tiled=True)
    up_all = lax.all_gather(shared_up, "tp", axis=1, tiled=True)
    down_all = lax.all_gather(shared_down, "tp", axis=0, tiled=True)
    ids_t = lax.all_gather(expert_ids.T, "z")
    weight_t = lax.all_gather(route_weight.T, "z")
    ids_t = lax.dynamic_index_in_dim(ids_t, column, 0, keepdims=False)
    weight_t = lax.dynamic_index_in_dim(weight_t, column, 0, keepdims=False)
    local = ids_t - plane * peers
    named = local[None] == jnp.arange(peers, dtype=jnp.int32)[:, None, None]
    member = jnp.any(named, axis=1)
    member_weight = jnp.sum(jnp.where(named, weight_t[None], 0.0), axis=1)
    spot = jnp.arange(token_count, dtype=jnp.int32)
    ahead = (spot[:, None] < spot[None, :]).astype(jnp.bfloat16)
    rank = jnp.dot(member.astype(jnp.bfloat16), ahead, preferred_element_type=jnp.float32)
    rank = jnp.where(member, rank.astype(jnp.int32), -1)
    slot = jnp.arange(capacity, dtype=jnp.int32)
    chosen = rank[:, None, :] == slot[None, :, None]
    pick = chosen.astype(jnp.bfloat16).reshape(peers * capacity, token_count)
    spread = (
        jnp.where(chosen, member_weight[:, None, :], 0.0)
        .astype(jnp.bfloat16)
        .reshape(peers * capacity, token_count)
    )

    mixer_out = mixer(
        mixer_input, document_ids, decay_rate, rotation, forget_log, input_map, readout_map, skip_gain
    )
    whole_rows = lax.all_to_all(mixer_out, "tp", split_axis=0, concat_axis=1, tiled=True)
    mixed = jnp.dot(whole_rows, out_projection, preferred_element_type=jnp.float32)
    residual = (stream.astype(jnp.float32) + mixed).astype(jnp.bfloat16)
    resid_f = residual.astype(jnp.float32)
    normed = (
        resid_f
        * lax.rsqrt(jnp.mean(resid_f * resid_f, axis=-1, keepdims=True) + norm_eps)
        * norm_gain[None, :]
    ).astype(jnp.bfloat16)
    model_width = normed.shape[1]

    gathered = lax.all_gather(normed, "z")
    tokens = lax.all_to_all(gathered, "tp", split_axis=0, concat_axis=0, tiled=True)
    tokens = tokens.reshape(token_count, model_width)
    rows = jnp.dot(pick, tokens, preferred_element_type=jnp.float32).astype(jnp.bfloat16)
    arrived = lax.all_to_all(
        rows.reshape(peers, capacity, model_width), ("x", "tp"), split_axis=0, concat_axis=0, tiled=True
    )
    row_block = arrived.reshape(-1, model_width)
    gate_value = jnp.dot(row_block, expert_gate[0], preferred_element_type=jnp.float32)
    up_value = jnp.dot(row_block, expert_up[0], preferred_element_type=jnp.float32)
    hidden = (jax.nn.silu(gate_value) * up_value).astype(jnp.bfloat16)
    expert_rows = jnp.dot(hidden, expert_down[0], preferred_element_type=jnp.float32).astype(
        jnp.bfloat16
    )
    returned = lax.all_to_all(
        expert_rows.reshape(arrived.shape), ("x", "tp"), split_axis=0, concat_axis=0, tiled=True
    )
    gate_block = jnp.dot(normed, gate_all, preferred_element_type=jnp.float32)
    up_block = jnp.dot(normed, up_all, preferred_element_type=jnp.float32)
    shared_hidden = (jax.nn.silu(gate_block) * up_block).astype(jnp.bfloat16)
    shared = jnp.dot(shared_hidden, down_all, preferred_element_type=jnp.float32)

    plane_sum = lax.dot_general(
        spread,
        returned.reshape(-1, model_width),
        (((0,), (0,)), ((), ())),
        preferred_element_type=jnp.float32,
    ).astype(jnp.bfloat16)
    back = lax.all_to_all(
        plane_sum.reshape(gathered.shape), "tp", split_axis=0, concat_axis=0, tiled=True
    )
    routed = lax.psum_scatter(back, "z", scatter_dimension=0, tiled=False)
    return (resid_f + shared + routed.astype(jnp.float32)).astype(jnp.bfloat16)


def solution(mesh):
    devices = mesh.devices
    planes = devices.shape[1]
    shape = (planes, devices.shape[0] // planes, devices.shape[1])
    split = Mesh(devices.reshape(shape), ("z", "x", "tp"))
    sp = ("z", "x")
    every = ("z", "x", "tp")
    placed = (
        P(every, None),
        P(sp, "tp"),
        P(sp),
        P("tp", None),
        P("tp", None),
        P(sp, "tp"),
        P(None, "tp", None, None),
        P(None, "tp", None, None),
        P("tp", None),
        P(),
        P(),
        P(sp, None),
        P(sp, None),
        P(every, None, None),
        P(every, None, None),
        P(every, None, None),
        P(None, "tp"),
        P(None, "tp"),
        P("tp", None),
    )
    return jax.shard_map(
        body, mesh=split, in_specs=placed, out_specs=P(every, None), check_vma=False
    )
```
